32 devices in a mesh: grp: 2 (over y), sp: 16 (over z, x, core), tp: 1.
Axes of the slice: x: 2, y: 2, z: 4, core: 2. Of those that a mesh axis runs over, the one named last changes fastest.
Arguments:
- resid: bfloat16 [8192, 2048], P(('grp', 'sp', 'tp')), parts along dimension 0, may hold values from -6 to 6
- gate_b: bfloat16 [8192, 2048], P(('grp', 'sp'), 'tp'), parts along dimension 0, may hold values from -6 to 6
- gate_c: bfloat16 [8192, 2048], P(('grp', 'sp'), 'tp'), parts along dimension 0, may hold values from -6 to 6
- value: bfloat16 [8192, 2048], P(('grp', 'sp'), 'tp'), parts along dimension 0, may hold values from -6 to 6
- taps: bfloat16 [3, 2048], P(None, 'tp'), may hold values from -3.5 to 3.5
- doc_ids: int32 [8192], P(('grp', 'sp')), parts along dimension 0, may hold values from 0 to 3, never falling along the last dimension, each value on 1 to 2048 neighbouring positions
- out_weight: bfloat16 [2048, 2048], P('tp'), may hold values from -0.125 to 0.125
- norm_gains: float32 [3, 2048], replicated, may hold values from 0.1 to 1.9
- routes: int32 [8192, 2], P(('grp', 'sp')), parts along dimension 0, may hold values from 0 to 15, all different within a row; in each aligned block of 256 rows (0 to 255, 256 to 511, ...) at most 48 rows name the same one
- route_weights: float32 [8192, 2], P(('grp', 'sp')), parts along dimension 0, may hold values from 0.2 to 1
- w_gate: bfloat16 [16, 2048, 4096], P('sp', None, 'tp'), may hold values from -0.125 to 0.125
- w_up: bfloat16 [16, 2048, 4096], P('sp', None, 'tp'), may hold values from -0.125 to 0.125
- w_down: bfloat16 [16, 4096, 2048], P('sp', 'tp'), may hold values from -0.09375 to 0.09375
Outputs:
- layer_out: bfloat16 [8192, 2048], P(('grp', 'sp', 'tp')), parts along dimension 0
The draws below stay inside these ranges and needn't reach their ends.
There are 2 independent parts, one for each index of `grp`. The reference program is written for one: setup_inputs(seed, part) draws one part's arguments, and reference() takes and returns one part's arrays. A program takes and returns all parts, laid end to end along the dimension named above; an argument that names none is the same for every part. Nothing has to cross between parts.
Inputs may be any that keep to these rules, and one draw needn't show every extreme that they name: `doc_ids`: never falling along the sequence; each document spans 1 to 2048 positions. `routes`: each row names 2 different experts. In each aligned block of 256 rows no expert is named more than 48 times, and in every draw some block names some expert exactly 48 times.
All inputs are finite; a program needn't handle non-finite values.
Results may differ from the reference program's by a relative error of at most 0.02.
Values may be sent and summed in bfloat16 or wider, within the bound.
A program may use at most 128 MiB of HBM per device.

```python
import math
import jax
import jax.numpy as jnp
import numpy as np
from jax import lax

D = 2048
FF = 4096
TAPS = 3
TOP = 2
TOKENS = 4096
ROWS_BLK = 256
EXPERTS = 16
CAP = 48
DOCS = 4
DOC_MOST = 2048
N_TP = 1


def steps_of(key, dims, cuts, least, high):
    loudness, own = 1.0, jax.random.fold_in(key, 6)
    for position, shards_of in cuts:
        steps = jnp.exp(jax.random.uniform(jax.random.fold_in(own, position), (shards_of,), jnp.float32, least / len(cuts), high / len(cuts)))
        loudness = loudness * jnp.repeat(steps, dims[position] // shards_of).reshape([-1 if axis == position else 1 for axis in range(len(dims))])
    return loudness


def profile(amount, total, most, lean):
    weights = [(1 << 20) // math.isqrt(rank ** lean) + 1 for rank in range(2, amount + 1)]
    rest, counts = total - most - (amount - 1), [1] * (amount - 1)
    while rest > 0:
        movable = [i for i in range(amount - 1) if counts[i] < most]
        whole, budget = sum([weights[i] for i in movable]), rest
        for i in movable:
            more = min(most - counts[i], max(1, budget * weights[i] // whole), rest)
            counts[i] = counts[i] + more
            rest = rest - more
    return np.array([most] + counts)


def uneven(rng, amount, total, reach, slope):
    if amount == 2:
        one = jax.random.randint(rng, (), max(1, total - reach), min(reach, total - 1) + 1)
        return jnp.stack([one, total - one])
    sizes = jnp.asarray(profile(amount, total, reach, slope), jnp.int32)
    twos = (amount - 1) // 2
    source_of, receiver = sizes[1:1 + 2 * twos:2], sizes[2:2 + 2 * twos:2]
    margin = jnp.minimum(source_of - 1, reach - receiver)
    shifted = jax.random.randint(jax.random.fold_in(rng, 1), (twos,), 0, 1 << 20) % (margin + 1)
    sizes = sizes.at[1:1 + 2 * twos:2].set(source_of - shifted).at[2:2 + 2 * twos:2].set(receiver + shifted)
    return sizes[jax.random.permutation(jax.random.fold_in(rng, 2), amount)]


def shared_out(rng, own, number, rows, amount, top, limit, lean):
    sequence = jax.random.permutation(rng, amount)
    packed, common = load_shares(amount, rows * top, limit, lean, True), load_shares(amount, rows * top, limit, lean, False)
    places = jnp.arange(amount)

    def named(lengths, offset_by):
        used = int((lengths > 0).sum())
        fixed = max(1, used // 4)
        shifted = fixed + (places - fixed + offset_by * (used - fixed)) % max(1, amount - fixed)
        return jnp.zeros((amount,), jnp.int32).at[sequence[jnp.where(places < fixed, places, shifted)]].set(jnp.asarray(lengths, jnp.int32))

    lengths = jnp.where(number % 4 == 0, named(packed, number // 4), named(common, number - number // 4 - 1))
    mixed = jax.random.permutation(jax.random.fold_in(own, 3), amount)
    giver, receiver = mixed[0:amount // 2 * 2:2], mixed[1:amount // 2 * 2:2]
    slack = jnp.minimum(lengths[giver] - 1, limit - lengths[receiver]) // 2
    slack = jnp.where((giver == sequence[0]) | (receiver == sequence[0]) | (lengths[receiver] == 0), 0, jnp.maximum(slack, 0))
    shifted = jax.random.randint(jax.random.fold_in(own, 4), (amount // 2,), 0, 1 << 20) % (slack + 1)
    lengths = lengths.at[giver].add(-shifted).at[receiver].add(shifted)
    members = jnp.searchsorted(jnp.cumsum(lengths), jnp.arange(rows * top), side="right").astype(jnp.int32)
    listing = members.reshape(top, rows).T
    listing = listing[jax.random.permutation(jax.random.fold_in(own, 1), rows)]
    offset_by = jax.random.randint(jax.random.fold_in(own, 2), (rows, 1), 0, top)
    return jnp.take_along_axis(listing, (jnp.arange(top)[None, :] + offset_by) % top, axis=1)


def load_shares(amount, total, most, skew, full):
    portions = [(1 << 20) // math.isqrt(standing ** skew) + 1 for standing in range(1, amount + 1)]
    largest = most if full else min(most, max(-(-total // amount), total * portions[0] // sum(portions)))
    least = 1 if total - largest >= amount - 1 else 0
    holding, spare = [largest] + [least] * (amount - 1), total - largest - least * (amount - 1)
    while spare > 0:
        free = [i for i in range(1, amount) if holding[i] < largest] or [i for i in range(1, amount) if holding[i] < most]
        mass, remaining = sum([portions[i] for i in free]), spare
        for i in free:
            extra = min(most - holding[i], max(1, remaining * portions[i] // mass), spare)
            holding[i] = holding[i] + extra
            spare = spare - extra
    return np.array(holding)


def bell_draw(rng, shape, deviation, limit, pieces=(), held_as=jnp.bfloat16):
    values = deviation * jax.random.normal(rng, shape, jnp.float32)
    if pieces:
        values = values * steps_of(rng, shape, pieces, -0.22, 0.18)
    return jnp.clip(values, -limit, limit).astype(held_as)


def setup_inputs(seed: int = 0, part: int = 0) -> dict:
    key_of = jax.random.split(jax.random.key(seed), 14)
    own_keys = jax.random.split(jax.random.fold_in(key_of[13], part), 14)
    resid = bell_draw(own_keys[0], (TOKENS, D), 1.0, 6.0, ((0, 16),))
    gate_b = bell_draw(own_keys[1], (TOKENS, D), 1.0, 6.0, ((0, 16),))
    gate_c = bell_draw(own_keys[2], (TOKENS, D), 1.0, 6.0, ((0, 16),))
    value = bell_draw(own_keys[3], (TOKENS, D), 1.0, 6.0, ((0, 16),))
    taps = bell_draw(key_of[4], (TAPS, D), TAPS ** -0.5, 3.5)
    doc_ids = jnp.searchsorted(jnp.cumsum(uneven(own_keys[5], DOCS, TOKENS, DOC_MOST, 1)), jnp.arange(TOKENS), side="right").astype(jnp.int32)
    out_weight = bell_draw(key_of[6], (D, D), D ** -0.5, 0.125)
    norm_gains = jnp.clip(1.0 + 0.18 * jax.random.normal(key_of[7], (3, D), jnp.float32), 0.1, 1.9)
    routes_keys = jax.random.split(jax.random.fold_in(own_keys[8], 1), TOKENS // ROWS_BLK)
    routes_turns = jax.random.permutation(jax.random.fold_in(own_keys[8], 3), TOKENS // ROWS_BLK)
    routes = jax.vmap(lambda own, number: shared_out(jax.random.fold_in(own_keys[8], 2), own, number, ROWS_BLK, EXPERTS, TOP, CAP, 1))(routes_keys, routes_turns).reshape((TOKENS, TOP))
    route_weights = jnp.clip(0.2 + 0.8 * jax.random.uniform(own_keys[9], (TOKENS, TOP), jnp.float32) ** steps_of(own_keys[9], (TOKENS, TOP), ((0, 16),), -0.2, 0.2), 0.2, 1.0)
    w_gate = bell_draw(key_of[10], (EXPERTS, D, FF), D ** -0.5, 0.125, ((0, 16),))
    w_up = bell_draw(key_of[11], (EXPERTS, D, FF), D ** -0.5, 0.125, ((0, 16),))
    w_down = bell_draw(key_of[12], (EXPERTS, FF, D), FF ** -0.5, 0.09375, ((0, 16),))
    return {"resid": resid, "gate_b": gate_b, "gate_c": gate_c, "value": value, "taps": taps, "doc_ids": doc_ids, "out_weight": out_weight, "norm_gains": norm_gains, "routes": routes, "route_weights": route_weights, "w_gate": w_gate, "w_up": w_up, "w_down": w_down}


norm_eps = 1e-06

def rms_scale(values, gain_row):
    mean_sq = lax.optimization_barrier(jnp.mean(values * values, axis=-1, keepdims=True))
    return values * lax.rsqrt(mean_sq + norm_eps) * gain_row

def slot_table(block_routes, experts, capacity):
    block_count = block_routes.shape[0]
    block_len = block_routes.shape[1]
    flat_routes = block_routes.reshape(block_count, block_len * TOP)
    onehot = (flat_routes[:, :, None] == jnp.arange(experts, dtype=jnp.int32)[None, None, :]).astype(jnp.int32)
    before = (jnp.cumsum(onehot, axis=1) - onehot).astype(jnp.int32)
    slot_rank = lax.optimization_barrier(jnp.sum(before * onehot, axis=2)).astype(jnp.int32)
    slot_hit = onehot[:, :, :, None] * (slot_rank[:, :, None, None] == jnp.arange(capacity, dtype=jnp.int32)[None, None, None, :]).astype(jnp.int32)
    owner_row = jnp.arange(block_len * TOP, dtype=jnp.int32) // TOP
    slot_tok = lax.optimization_barrier(jnp.sum(slot_hit * owner_row[None, :, None, None], axis=1)).astype(jnp.int32)
    filled = lax.optimization_barrier(jnp.sum(slot_hit, axis=1)).astype(jnp.int32)
    return (slot_rank.reshape(block_count, block_len, TOP), slot_tok, filled)

def grouped_product(left_rows, right_rows, groups):
    group_width = left_rows.shape[1] // groups

    def add_group(running, group_index):
        first = group_index * group_width
        block_cols = lax.dynamic_slice_in_dim(left_rows, first, group_width, 1)
        block_rows = lax.dynamic_slice_in_dim(right_rows, first, group_width, 0)
        group_term = jnp.dot(block_cols, block_rows, preferred_element_type=jnp.float32).astype(jnp.bfloat16)
        group_term = lax.optimization_barrier(group_term)
        return (running + group_term.astype(jnp.float32), None)
    start_sum = jnp.zeros((left_rows.shape[0], right_rows.shape[1]), jnp.float32)
    running, _ = lax.scan(add_group, start_sum, jnp.arange(groups, dtype=jnp.int32))
    return running

def reference(resid, gate_b, gate_c, value, taps, doc_ids, out_weight, norm_gains, routes, route_weights, w_gate, w_up, w_down):
    product = gate_c.astype(jnp.float32) * value.astype(jnp.float32)
    tap_weights = taps.astype(jnp.float32)
    convolved = tap_weights[0] * product
    for distance in range(1, TAPS):
        earlier = jnp.pad(product, ((distance, 0), (0, 0)))[:TOKENS]
        earlier_ids = jnp.pad(doc_ids, (distance, 0), constant_values=-1)[:TOKENS]
        same_doc = earlier_ids == doc_ids
        convolved = convolved + jnp.where(same_doc[:, None], tap_weights[distance] * earlier, 0.0)
    mixed_rows = (gate_b.astype(jnp.float32) * convolved).astype(jnp.bfloat16)
    projected = grouped_product(mixed_rows, out_weight, N_TP)
    gain_rows = norm_gains.astype(jnp.float32)
    stream = resid.astype(jnp.float32) + rms_scale(projected, gain_rows[0])
    normed = rms_scale(stream, gain_rows[1]).astype(jnp.bfloat16)
    blocks = TOKENS // ROWS_BLK
    slot_rank, slot_tok, filled = slot_table(routes.reshape(blocks, ROWS_BLK, TOP), EXPERTS, CAP)
    normed_blocks = normed.reshape(blocks, ROWS_BLK, D)

    def one_expert(expert):
        slot_picks = slot_tok[:, expert]
        slot_live = filled[:, expert]
        picked_rows = jax.vmap(lambda block_rows, picks: block_rows[picks])(normed_blocks, slot_picks)
        picked_rows = jnp.where(slot_live[:, :, None] > 0, picked_rows, jnp.zeros_like(picked_rows))
        picked_rows = picked_rows.reshape(blocks * CAP, D)
        gate_proj = jnp.dot(picked_rows, w_gate[expert], preferred_element_type=jnp.float32)
        up_proj = jnp.dot(picked_rows, w_up[expert], preferred_element_type=jnp.float32)
        hidden = (jax.nn.silu(gate_proj) * up_proj).astype(jnp.bfloat16)
        expert_out = grouped_product(hidden, w_down[expert], N_TP).astype(jnp.bfloat16)
        return expert_out.reshape(blocks, CAP, D)
    expert_out = lax.map(one_expert, jnp.arange(EXPERTS, dtype=jnp.int32))
    block_index = jnp.arange(TOKENS, dtype=jnp.int32) // ROWS_BLK
    picked = expert_out[routes, block_index[:, None], slot_rank.reshape(TOKENS, TOP)]
    shares = route_weights / lax.optimization_barrier(jnp.sum(route_weights, axis=1, keepdims=True))
    combined = lax.optimization_barrier(jnp.sum(shares[:, :, None] * picked.astype(jnp.float32), axis=1))
    return (stream + rms_scale(combined, gain_rows[2])).astype(jnp.bfloat16)
```

```python
import functools

import jax
import jax.numpy as jnp
import numpy as np
from jax import lax
from jax.experimental import pallas as pl
from jax.experimental.pallas import tpu as pltpu
from jax.sharding import PartitionSpec as P

TAPS = 3
TOP = 2


norm_eps = 1e-06


def passed_along(block, axis, distance):
    devices = range(lax.axis_size(axis))
    route = [(i - distance, i) for i in devices if i - distance in devices]
    return lax.ppermute(block, axis, route)


def rms_scale(values, gain_row):
    mean_sq = jnp.mean(values * values, axis=-1, keepdims=True)
    return values * lax.rsqrt(mean_sq + norm_eps) * gain_row


def slot_table(block_routes, experts, capacity):
    block_count = block_routes.shape[0]
    block_len = block_routes.shape[1]
    flat_routes = block_routes.reshape(block_count, block_len * TOP)
    onehot = (
        flat_routes[:, :, None] == jnp.arange(experts, dtype=jnp.int32)[None, None, :]
    ).astype(jnp.int32)
    before = jnp.cumsum(onehot, axis=1) - onehot
    slot_rank = jnp.sum(before * onehot, axis=2)
    slot_hit = onehot[:, :, :, None] * (
        slot_rank[:, :, None, None] == jnp.arange(capacity, dtype=jnp.int32)[None, None, None, :]
    ).astype(jnp.int32)
    owner_row = jnp.arange(block_len * TOP, dtype=jnp.int32) // TOP
    slot_tok = jnp.sum(slot_hit * owner_row[None, :, None, None], axis=1)
    filled = jnp.sum(slot_hit, axis=1)
    return (slot_rank.reshape(block_count, block_len, TOP), slot_tok, filled)


def pick_rows(normed_rows, slot_tok, filled):
    picked_rows = normed_rows[slot_tok]
    return jnp.where(filled[:, :, None] > 0, picked_rows, jnp.zeros_like(picked_rows))


def expert_hidden(picked_rows, w_gate, w_up):
    gate_proj = jnp.dot(picked_rows, w_gate[0], preferred_element_type=jnp.float32)
    up_proj = jnp.dot(picked_rows, w_up[0], preferred_element_type=jnp.float32)
    return (jax.nn.silu(gate_proj) * up_proj).astype(jnp.bfloat16)


def per_device_split(
    resid,
    gate_b,
    gate_c,
    value,
    taps,
    doc_ids,
    out_weight,
    norm_gains,
    routes,
    route_weights,
    w_gate,
    w_up,
    w_down,
):
    tok_dev = gate_b.shape[0]
    rows_blk = resid.shape[0]
    model_width = resid.shape[1]
    experts = lax.axis_size("sp")
    capacity = max(2, 3 * TOP * rows_blk // (2 * experts))
    tap_reach = TAPS - 1
    product = gate_c.astype(jnp.float32) * value.astype(jnp.float32)
    id_values = doc_ids.astype(jnp.float32)
    prev_rows, prev_ids = passed_along(
        (product[tok_dev - tap_reach :], id_values[tok_dev - tap_reach :]), "sp", 1
    )
    ext_rows = jnp.concatenate([prev_rows, product], axis=0)
    ext_ids = jnp.concatenate([prev_ids, id_values], axis=0)
    tap_weights = taps.astype(jnp.float32)
    convolved = tap_weights[0] * product
    for distance in range(1, TAPS):
        earlier = ext_rows[tap_reach - distance : tap_reach - distance + tok_dev]
        same_doc = ext_ids[tap_reach - distance : tap_reach - distance + tok_dev] == id_values
        convolved = convolved + jnp.where(same_doc[:, None], tap_weights[distance] * earlier, 0.0)
    mixed_rows = (gate_b.astype(jnp.float32) * convolved).astype(jnp.bfloat16)
    block_rows = mixed_rows
    projected = lax.psum_scatter(
        jnp.dot(block_rows, out_weight, preferred_element_type=jnp.float32).astype(jnp.bfloat16),
        "tp",
        scatter_dimension=0,
        tiled=True,
    ).astype(jnp.float32)
    stream = resid.astype(jnp.float32) + rms_scale(projected, norm_gains[0])
    normed = rms_scale(stream, norm_gains[1]).astype(jnp.bfloat16)
    lane_index = lax.axis_index("tp")
    offset = lane_index * rows_blk
    my_routes = lax.dynamic_slice_in_dim(routes, offset, rows_blk, 0)
    my_weights = lax.dynamic_slice_in_dim(route_weights, offset, rows_blk, 0)
    own_rank, own_tok, own_filled = slot_table(my_routes[None], experts, capacity)
    slot_rank = own_rank[0]
    outgoing = pick_rows(normed, own_tok[0], own_filled[0])
    arrived = lax.all_to_all(outgoing, "sp", split_axis=0, concat_axis=0, tiled=True)
    hidden = expert_hidden(
        lax.all_gather(arrived[None], "tp", axis=0, tiled=True).reshape(-1, model_width),
        w_gate,
        w_up,
    )
    block_rows = hidden
    summed = lax.psum_scatter(
        jnp.dot(block_rows, w_down[0], preferred_element_type=jnp.float32).astype(jnp.bfloat16),
        "tp",
        scatter_dimension=0,
        tiled=True,
    )
    results = summed.reshape(experts, capacity, model_width)
    returned = lax.all_to_all(results, "sp", split_axis=0, concat_axis=0, tiled=True)
    picked = returned[my_routes, slot_rank]
    shares = my_weights / jnp.sum(my_weights, axis=1, keepdims=True)
    combined = jnp.sum(shares[:, :, None] * picked.astype(jnp.float32), axis=1)
    return (stream + rms_scale(combined, norm_gains[2])).astype(jnp.bfloat16)


MESH = pl.DeviceIdType.MESH


def flipped(me, distance, n):
    out, bit = 0, 1
    while bit < n:
        digit = (me // bit) % 2
        if distance & bit:
            digit = 1 - digit
        out = out + digit * bit
        bit *= 2
    return out


def expert_kernel(
    n, cap, tile, down_tile, chunk,
    rows_hbm, normed_hbm, meta_hbm, gate_hbm, up_hbm, down_hbm,
    weights_v, spread_v, spread_t, wanted_row, wanted_col, stream_hbm, gain_v, out_v,
    gate_v, up_v, down_v, arrived, hidden, near_back, far_sum, tokens, picked, relay_back,
    meta_v, chosen_t, relay_weights, stream_v, total,
    gate_sem, up_sem, down_sem, tok_send, tok_recv, meta_send, meta_recv,
    near_send, near_recv, pick_send, pick_recv, back_send, back_recv,
    far_send, far_recv, sum_send, sum_recv, own_sem,
):
    me = lax.axis_index("sp")
    quarter, half = n // 4, n // 2
    plane, spot = me // quarter, me % quarter
    side = plane // 2
    relaying = (plane + side) % 2
    units = gate_v.shape[1]
    width = normed_hbm.shape[1]
    depth = down_v.shape[0]
    chunks = width // chunk
    down_tiles = width // down_tile
    far_relay = (2 - side) * quarter + spot
    my_turn = 1 - relaying

    def source_of(s):
        return ((2 - side) + s * (1 - 2 * side)) * quarter + spot

    def columns(t, size):
        return pl.ds(pl.multiple_of(t * size, size), size)

    def load(src, dst, sem, t, size):
        cols = columns(t, size)
        return pltpu.make_async_copy(src.at[0, :, cols], dst.at[:, cols], sem.at[t])

    def load_down(step):
        return pltpu.make_async_copy(
            down_hbm.at[0, :, columns(step % down_tiles, down_tile)],
            down_v.at[step % depth],
            down_sem.at[step % depth],
        )

    def remote(src, dst, sent, got, device):
        return pltpu.make_async_remote_copy(
            src_ref=src, dst_ref=dst, send_sem=sent, recv_sem=got,
            device_id={"sp": device}, device_id_type=MESH,
        )

    def settle(ref, sem):
        pltpu.make_async_copy(ref, ref, sem).wait()

    def block(i, count=1):
        return pl.ds(i * cap, count * cap)

    barrier = pltpu.get_barrier_semaphore()

    def greet(device):
        pl.semaphore_signal(barrier, inc=1, device_id={"sp": device}, device_id_type=MESH)

    for d in range(1, half):
        greet(flipped(me, d, n))
    greet(far_relay)

    @pl.when(relaying == 1)
    def _():
        greet(source_of(0))
        greet(source_of(1))

    own_rows = pltpu.make_async_copy(rows_hbm.at[block(0)], arrived.at[block(0)], own_sem.at[0])
    own_rows.start()
    for t in range(units // tile):
        load(gate_hbm, gate_v, gate_sem, t, tile).start()
        load(up_hbm, up_v, up_sem, t, tile).start()
    for t in range(depth):
        load_down(t).start()
    stream_in = pltpu.make_async_copy(stream_hbm, stream_v, own_sem.at[1])
    stream_in.start()
    pl.semaphore_wait(barrier, half + 2 * relaying)

    def send_tokens():
        remote(
            meta_hbm, meta_v.at[my_turn], meta_send.at[0], meta_recv.at[my_turn], far_relay
        ).start()
        for c in range(chunks):
            cols = pl.ds(c * chunk, chunk)
            remote(
                normed_hbm.at[:, cols], tokens.at[my_turn, :, cols],
                tok_send.at[0], tok_recv.at[my_turn * chunks + c], far_relay,
            ).start()

    def send_near(distances):
        for d in distances:
            remote(
                rows_hbm.at[block(d)], arrived.at[block(d)],
                near_send.at[0], near_recv.at[d // quarter], flipped(me, d, n),
            ).start()

    @pl.when(relaying == 1)
    def _():
        send_tokens()

    send_near(list(range(1, quarter)) + list(range(quarter, half)))

    @pl.when(relaying == 0)
    def _():
        send_tokens()

    def pick(s, c):
        cols = columns(c, chunk)
        settle(tokens.at[s, :, cols], tok_recv.at[s * chunks + c])
        if s > 0:
            settle(picked.at[block(1, half - 1), cols], pick_send.at[c])
        rows = jnp.dot(
            chosen_t[...], tokens[s, :, cols], preferred_element_type=jnp.float32
        ).astype(jnp.bfloat16)
        arrived[block(half + s * quarter), cols] = rows[:cap]
        picked[pl.ds(cap, (half - 1) * cap), cols] = rows[cap:]
        for d in list(range(quarter, half)) + list(range(1, quarter)):
            remote(
                picked.at[block(d), cols],
                arrived.at[block(half + s * quarter + d % quarter), cols],
                pick_send.at[c], pick_recv.at[s * chunks + c], flipped(me, d, n),
            ).start()

    def read_meta(s):
        settle(meta_v.at[s], meta_recv.at[s])
        places = meta_v[s, :half].astype(jnp.bfloat16)
        shares = meta_v[s, half:].astype(jnp.bfloat16)
        chosen_t[...] = (
            jnp.dot(spread_t[...], places, preferred_element_type=jnp.float32) == wanted_col[...]
        ).astype(jnp.float32).astype(jnp.bfloat16)
        across = (((0,), (0,)), ((), ()))
        slots = lax.dot_general(places, spread_v[...], across, preferred_element_type=jnp.float32)
        spread_shares = lax.dot_general(
            shares, spread_v[...], across, preferred_element_type=jnp.float32
        )
        relay_weights[s] = jnp.where(slots == wanted_row[...], spread_shares, 0.0).astype(
            jnp.bfloat16
        )

    def relay_sum(s, c):
        cols = columns(c, chunk)
        settle(relay_back.at[s, block(1, half - 1), cols], far_recv.at[s * chunks + c])
        tokens[s, :, cols] = jnp.dot(
            relay_weights[s], relay_back[s, :, cols], preferred_element_type=jnp.float32
        ).astype(jnp.bfloat16)
        remote(
            tokens.at[s, :, cols], far_sum.at[:, cols], sum_send.at[0], sum_recv.at[c], source_of(s)
        ).start()

    def on_relay(task):
        pl.when(relaying == 1)(task)

    def experts(g, halfway=None, between=None):
        rows = block(g * quarter, quarter)
        far = g >= 2
        s = g - 2

        @pl.loop(0, units // tile)
        def _(t):
            if halfway is not None:
                pl.when((relaying == 1) & (t == units // tile // 2))(halfway)
            if g == 0:
                load(gate_hbm, gate_v, gate_sem, t, tile).wait()
                load(up_hbm, up_v, up_sem, t, tile).wait()
            cols = columns(t, tile)
            x = arrived[rows, :]
            gate = jnp.dot(x, gate_v[:, cols], preferred_element_type=jnp.float32)
            up = jnp.dot(x, up_v[:, cols], preferred_element_type=jnp.float32)
            hidden[:, cols] = (gate / (1.0 + jnp.exp(-gate)) * up).astype(jnp.bfloat16)

        if between is not None:
            on_relay(between)

        @pl.loop(0, down_tiles)
        def _(t):
            step = g * down_tiles + t
            load_down(step).wait()
            cols = columns(t, down_tile)
            result = jnp.dot(
                hidden[...], down_v[step % depth], preferred_element_type=jnp.float32
            ).astype(jnp.bfloat16)
            arrived[rows, cols] = result
            if g == 0:
                near_back[block(0), cols] = result[:cap]

            if far:
                @pl.when(relaying == 1)
                def _():
                    relay_back[s, block(0), cols] = result[:cap]

            @pl.when(step + depth < 4 * down_tiles)
            def _():
                load_down(step + depth).start()

            if far:
                per = chunk // down_tile

                @pl.when(t % per == per - 1)
                def _():
                    c = t // per
                    wide = columns(c, chunk)

                    def give(p):
                        target = (1 + side) * quarter + flipped(spot, p, quarter)
                        place = pl.multiple_of((p + quarter * (1 - relaying)) * cap, cap)
                        remote(
                            arrived.at[block(g * quarter + p), wide],
                            relay_back.at[s, pl.ds(place, cap), wide],
                            far_send.at[s], far_recv.at[s * chunks + c], target,
                        ).start()

                    pl.when(relaying == 0)(functools.partial(give, 0))
                    for p in range(1, quarter):
                        give(p)

        if not far:
            for d in range(max(1, g * quarter), (g + 1) * quarter):
                remote(
                    arrived.at[block(d)], near_back.at[block(d)],
                    back_send.at[g], back_recv.at[g], flipped(me, d, n),
                ).start()

    def first_pick():
        read_meta(0)
        pick(0, 0)

    def second_pick():
        pick(0, chunks - 1)
        read_meta(1)

    on_relay(first_pick)
    own_rows.wait()
    settle(arrived.at[block(1, quarter - 1)], near_recv.at[0])
    experts(0, halfway=lambda: pick(0, 1), between=lambda: pick(0, 2))
    on_relay(second_pick)
    settle(arrived.at[block(quarter, quarter)], near_recv.at[1])
    experts(1, halfway=lambda: pick(1, 0), between=lambda: pick(1, 1))

    def await_far(s):
        first = half + s * quarter

        @pl.when(relaying == 1)
        def _():
            for c in range(chunks):
                cols = pl.ds(c * chunk, chunk)
                settle(arrived.at[block(first + 1, quarter - 1), cols], pick_recv.at[s * chunks + c])

        @pl.when(relaying == 0)
        def _():
            for c in range(chunks):
                cols = pl.ds(c * chunk, chunk)
                settle(arrived.at[block(first, quarter), cols], pick_recv.at[s * chunks + c])

    await_far(0)
    experts(2, halfway=lambda: pick(1, 2))
    on_relay(lambda: pick(1, chunks - 1))

    def relay_sums(s):
        @pl.loop(0, chunks)
        def _(c):
            relay_sum(s, c)

    on_relay(lambda: relay_sums(0))
    settle(near_back.at[block(1, quarter - 1)], back_recv.at[0])
    settle(near_back.at[block(quarter, quarter)], back_recv.at[1])

    @pl.loop(0, chunks)
    def _(c):
        cols = columns(c, chunk)
        total[:, cols] = jnp.dot(
            weights_v[...], near_back[:, cols], preferred_element_type=jnp.float32
        )

    await_far(1)
    experts(3)
    on_relay(lambda: relay_sums(1))
    stream_in.wait()
    for c in range(chunks):
        cols = pl.ds(c * chunk, chunk)
        settle(far_sum.at[:, cols], sum_recv.at[c])

    part = 32

    @pl.loop(0, total.shape[0] // part)
    def _(t):
        some = pl.ds(pl.multiple_of(t * part, part), part)
        combined = total[some, :] + far_sum[some, :].astype(jnp.float32)
        out_v[some, :] = (stream_v[some, :] + rms_scale(combined, gain_v[...])).astype(out_v.dtype)

    settle(normed_hbm, tok_send.at[0])
    settle(meta_hbm, meta_send.at[0])
    settle(rows_hbm.at[block(1, half - 1)], near_send.at[0])
    settle(arrived.at[block(1, quarter - 1)], back_send.at[0])
    settle(arrived.at[block(quarter, quarter)], back_send.at[1])

    @pl.when(relaying == 1)
    def _():
        for c in range(chunks):
            settle(picked.at[block(1, half - 1), pl.ds(c * chunk, chunk)], pick_send.at[c])
        settle(tokens, sum_send.at[0])
        for s in range(2):
            settle(arrived.at[block(half + s * quarter + 1, quarter - 1)], far_send.at[s])

    @pl.when(relaying == 0)
    def _():
        for s in range(2):
            settle(arrived.at[block(half + s * quarter, quarter)], far_send.at[s])


def run_experts(outgoing, normed, meta, w_gate, w_up, w_down, weights, stream, gain, n, cap):
    model_width, units = w_gate.shape[1], w_gate.shape[2]
    rows_blk = normed.shape[0]
    tile, down_tile, chunk, depth = 256, 256, model_width // 4, 4
    half, chunks = n // 2, 4
    total_rows = n * cap
    slots = np.arange(half * cap)
    spread = (slots[None, :] // cap == np.arange(half)[:, None]).astype(np.float32)
    wanted = (slots % cap + 1).astype(np.float32)
    constants = (
        jnp.asarray(spread, jnp.bfloat16),
        jnp.asarray(spread.T, jnp.bfloat16),
        jnp.asarray(wanted[None, :]),
        jnp.asarray(wanted[:, None]),
    )
    dma = pltpu.SemaphoreType.DMA
    vmem = pltpu.VMEM
    anywhere = pl.BlockSpec(memory_space=pl.ANY)
    near = pl.BlockSpec(memory_space=pltpu.VMEM)
    return pl.pallas_call(
        functools.partial(expert_kernel, n, cap, tile, down_tile, chunk),
        out_shape=jax.ShapeDtypeStruct(stream.shape, jnp.bfloat16),
        in_specs=[anywhere] * 6 + [near] * 5 + [anywhere, near],
        out_specs=near,
        scratch_shapes=[
            vmem((model_width, units), jnp.bfloat16),
            vmem((model_width, units), jnp.bfloat16),
            vmem((depth, units, down_tile), jnp.bfloat16),
            vmem((total_rows, model_width), jnp.bfloat16),
            vmem((n // 4 * cap, units), jnp.bfloat16),
            vmem((half * cap, model_width), jnp.bfloat16),
            vmem((rows_blk, model_width), jnp.bfloat16),
            vmem((2, rows_blk, model_width), jnp.bfloat16),
            vmem((half * cap, model_width), jnp.bfloat16),
            vmem((2, half * cap, model_width), jnp.bfloat16),
            vmem((2,) + meta.shape, jnp.float32),
            vmem((half * cap, rows_blk), jnp.bfloat16),
            vmem((2, rows_blk, half * cap), jnp.bfloat16),
            vmem(stream.shape, jnp.float32),
            vmem(stream.shape, jnp.float32),
            dma((units // tile,)),
            dma((units // tile,)),
            dma((depth,)),
            dma((1,)),
            dma((2 * chunks,)),
            dma((1,)),
            dma((2,)),
            dma((1,)),
            dma((2,)),
            dma((chunks,)),
            dma((2 * chunks,)),
            dma((2,)),
            dma((2,)),
            dma((2,)),
            dma((2 * chunks,)),
            dma((1,)),
            dma((chunks,)),
            dma((2,)),
        ],
        compiler_params=pltpu.CompilerParams(
            collective_id=0, has_side_effects=True, vmem_limit_bytes=67043328
        ),
        cost_estimate=pl.CostEstimate(
            flops=6 * total_rows * model_width * units,
            bytes_accessed=6 * model_width * units,
            transcendentals=total_rows * units,
        ),
    )(outgoing, normed, meta, w_gate, w_up, w_down, weights, *constants, stream, gain)


def per_device_whole(
    resid, gate_b, gate_c, value, taps, doc_ids, out_weight, norm_gains,
    routes, route_weights, w_gate, w_up, w_down,
):
    tok_dev = gate_b.shape[0]
    rows_blk, model_width = resid.shape
    experts = lax.axis_size("sp")
    capacity = max(2, 3 * TOP * rows_blk // (2 * experts))
    tap_reach = TAPS - 1
    product = gate_c.astype(jnp.float32) * value.astype(jnp.float32)
    id_values = doc_ids.astype(jnp.float32)
    id_row = jnp.pad(id_values[tok_dev - tap_reach :], (0, model_width - tap_reach))
    handed = passed_along(
        jnp.concatenate([product[tok_dev - tap_reach :], id_row[None]], axis=0), "sp", 1
    )
    ext_rows = jnp.concatenate([handed[:tap_reach], product], axis=0)
    ext_ids = jnp.concatenate([handed[tap_reach, :tap_reach], id_values], axis=0)
    tap_weights = taps.astype(jnp.float32)
    convolved = tap_weights[0] * product
    for distance in range(1, TAPS):
        earlier = ext_rows[tap_reach - distance : tap_reach - distance + tok_dev]
        same_doc = ext_ids[tap_reach - distance : tap_reach - distance + tok_dev] == id_values
        convolved = convolved + jnp.where(same_doc[:, None], tap_weights[distance] * earlier, 0.0)
    mixed_rows = (gate_b.astype(jnp.float32) * convolved).astype(jnp.bfloat16)
    projected = (
        jnp.dot(mixed_rows, out_weight, preferred_element_type=jnp.float32)
        .astype(jnp.bfloat16)
        .astype(jnp.float32)
    )
    stream = resid.astype(jnp.float32) + rms_scale(projected, norm_gains[0])
    normed = rms_scale(stream, norm_gains[1]).astype(jnp.bfloat16)

    def dot32(a, b):
        return jnp.dot(a, b, preferred_element_type=jnp.float32)

    me = lax.axis_index("sp")
    quarter, half = experts // 4, experts // 2
    plane = me // quarter
    far_relay = (2 - plane // 2) * quarter + me % quarter
    places = jnp.arange(half, dtype=jnp.int32)
    visited = jnp.concatenate([places ^ me, places ^ far_relay])
    names = routes[:, :, None] == visited[None, None, :]
    hit = jnp.any(names, axis=1)
    earlier_rows = jnp.asarray(np.tril(np.ones((rows_blk, rows_blk), np.float32), -1), jnp.bfloat16)
    rank = dot32(earlier_rows, hit.astype(jnp.bfloat16))
    place = jnp.where(hit, rank + 1.0, 0.0)
    slots = np.arange(half * capacity)
    spread = jnp.asarray(
        (slots[None, :] // capacity == np.arange(half)[:, None]).astype(np.float32), jnp.bfloat16
    )
    wanted = jnp.asarray((slots % capacity + 1).astype(np.float32))
    chosen = dot32(place[:, :half].astype(jnp.bfloat16), spread) == wanted[None, :]
    outgoing = lax.dot_general(
        chosen.astype(jnp.bfloat16),
        normed,
        (((0,), (0,)), ((), ())),
        preferred_element_type=jnp.float32,
    ).astype(jnp.bfloat16)
    shares = route_weights / jnp.sum(route_weights, axis=1, keepdims=True)
    share_of = jnp.sum(jnp.where(names, shares[:, :, None], 0.0), axis=1)
    weights = jnp.where(
        chosen, dot32(share_of[:, :half].astype(jnp.bfloat16), spread), 0.0
    ).astype(jnp.bfloat16)
    meta = jnp.concatenate([place[:, half:].T, share_of[:, half:].T], axis=0)
    return run_experts(
        outgoing, normed, meta, w_gate, w_up, w_down, weights, stream, norm_gains[2:3], experts, capacity
    )


def solution(mesh):
    experts = mesh.shape["sp"]
    whole_tokens = mesh.shape["tp"] == 1 and experts >= 8 and experts & (experts - 1) == 0
    per_device = per_device_whole if whole_tokens else per_device_split
    return jax.shard_map(
        per_device,
        mesh=mesh,
        in_specs=(
            P(("grp", "sp", "tp"), None),
            P(("grp", "sp"), "tp"),
            P(("grp", "sp"), "tp"),
            P(("grp", "sp"), "tp"),
            P(None, "tp"),
            P(("grp", "sp")),
            P("tp", None),
            P(),
            P(("grp", "sp"), None),
            P(("grp", "sp"), None),
            P("sp", None, "tp"),
            P("sp", None, "tp"),
            P("sp", "tp", None),
        ),
        out_specs=P(("grp", "sp", "tp"), None),
        check_vma=False,
    )
```

```python
import functools

import jax
import jax.numpy as jnp
import numpy as np
from jax import lax
from jax.experimental import pallas as pl
from jax.experimental.pallas import tpu as pltpu
from jax.sharding import PartitionSpec as P

TAPS = 3
TOP = 2


norm_eps = 1e-06


def passed_along(block, axis, distance):
    devices = range(lax.axis_size(axis))
    route = [(i - distance, i) for i in devices if i - distance in devices]
    return lax.ppermute(block, axis, route)


def rms_scale(values, gain_row):
    mean_sq = jnp.mean(values * values, axis=-1, keepdims=True)
    return values * lax.rsqrt(mean_sq + norm_eps) * gain_row


def slot_table(block_routes, experts, capacity):
    block_count = block_routes.shape[0]
    block_len = block_routes.shape[1]
    flat_routes = block_routes.reshape(block_count, block_len * TOP)
    onehot = (
        flat_routes[:, :, None] == jnp.arange(experts, dtype=jnp.int32)[None, None, :]
    ).astype(jnp.int32)
    before = jnp.cumsum(onehot, axis=1) - onehot
    slot_rank = jnp.sum(before * onehot, axis=2)
    slot_hit = onehot[:, :, :, None] * (
        slot_rank[:, :, None, None] == jnp.arange(capacity, dtype=jnp.int32)[None, None, None, :]
    ).astype(jnp.int32)
    owner_row = jnp.arange(block_len * TOP, dtype=jnp.int32) // TOP
    slot_tok = jnp.sum(slot_hit * owner_row[None, :, None, None], axis=1)
    filled = jnp.sum(slot_hit, axis=1)
    return (slot_rank.reshape(block_count, block_len, TOP), slot_tok, filled)


def pick_rows(normed_rows, slot_tok, filled):
    picked_rows = normed_rows[slot_tok]
    return jnp.where(filled[:, :, None] > 0, picked_rows, jnp.zeros_like(picked_rows))


def expert_hidden(picked_rows, w_gate, w_up):
    gate_proj = jnp.dot(picked_rows, w_gate[0], preferred_element_type=jnp.float32)
    up_proj = jnp.dot(picked_rows, w_up[0], preferred_element_type=jnp.float32)
    return (jax.nn.silu(gate_proj) * up_proj).astype(jnp.bfloat16)


def per_device_split(
    resid,
    gate_b,
    gate_c,
    value,
    taps,
    doc_ids,
    out_weight,
    norm_gains,
    routes,
    route_weights,
    w_gate,
    w_up,
    w_down,
):
    tok_dev = gate_b.shape[0]
    rows_blk = resid.shape[0]
    model_width = resid.shape[1]
    experts = lax.axis_size("sp")
    capacity = max(2, 3 * TOP * rows_blk // (2 * experts))
    tap_reach = TAPS - 1
    product = gate_c.astype(jnp.float32) * value.astype(jnp.float32)
    id_values = doc_ids.astype(jnp.float32)
    prev_rows, prev_ids = passed_along(
        (product[tok_dev - tap_reach :], id_values[tok_dev - tap_reach :]), "sp", 1
    )
    ext_rows = jnp.concatenate([prev_rows, product], axis=0)
    ext_ids = jnp.concatenate([prev_ids, id_values], axis=0)
    tap_weights = taps.astype(jnp.float32)
    convolved = tap_weights[0] * product
    for distance in range(1, TAPS):
        earlier = ext_rows[tap_reach - distance : tap_reach - distance + tok_dev]
        same_doc = ext_ids[tap_reach - distance : tap_reach - distance + tok_dev] == id_values
        convolved = convolved + jnp.where(same_doc[:, None], tap_weights[distance] * earlier, 0.0)
    mixed_rows = (gate_b.astype(jnp.float32) * convolved).astype(jnp.bfloat16)
    block_rows = mixed_rows
    projected = lax.psum_scatter(
        jnp.dot(block_rows, out_weight, preferred_element_type=jnp.float32).astype(jnp.bfloat16),
        "tp",
        scatter_dimension=0,
        tiled=True,
    ).astype(jnp.float32)
    stream = resid.astype(jnp.float32) + rms_scale(projected, norm_gains[0])
    normed = rms_scale(stream, norm_gains[1]).astype(jnp.bfloat16)
    lane_index = lax.axis_index("tp")
    offset = lane_index * rows_blk
    my_routes = lax.dynamic_slice_in_dim(routes, offset, rows_blk, 0)
    my_weights = lax.dynamic_slice_in_dim(route_weights, offset, rows_blk, 0)
    own_rank, own_tok, own_filled = slot_table(my_routes[None], experts, capacity)
    slot_rank = own_rank[0]
    outgoing = pick_rows(normed, own_tok[0], own_filled[0])
    arrived = lax.all_to_all(outgoing, "sp", split_axis=0, concat_axis=0, tiled=True)
    hidden = expert_hidden(
        lax.all_gather(arrived[None], "tp", axis=0, tiled=True).reshape(-1, model_width),
        w_gate,
        w_up,
    )
    block_rows = hidden
    summed = lax.psum_scatter(
        jnp.dot(block_rows, w_down[0], preferred_element_type=jnp.float32).astype(jnp.bfloat16),
        "tp",
        scatter_dimension=0,
        tiled=True,
    )
    results = summed.reshape(experts, capacity, model_width)
    returned = lax.all_to_all(results, "sp", split_axis=0, concat_axis=0, tiled=True)
    picked = returned[my_routes, slot_rank]
    shares = my_weights / jnp.sum(my_weights, axis=1, keepdims=True)
    combined = jnp.sum(shares[:, :, None] * picked.astype(jnp.float32), axis=1)
    return (stream + rms_scale(combined, norm_gains[2])).astype(jnp.bfloat16)


MESH = pl.DeviceIdType.MESH


def flipped(me, distance, n):
    out, bit = 0, 1
    while bit < n:
        digit = (me // bit) % 2
        if distance & bit:
            digit = 1 - digit
        out = out + digit * bit
        bit *= 2
    return out


def pass_plan(n):
    quarter, half = n // 4, n // 2
    return [(range(quarter), None), ((), 0), (range(quarter, half), None), ((), 1)]


def expert_kernel(
    n, cap, tile, down_tile, chunk,
    rows_hbm, normed_hbm, meta_hbm, gate_hbm, up_hbm, down_hbm,
    weights_v, spread_v, spread_t, wanted_row, wanted_col, stream_hbm, gain_v, out_v,
    gate_v, up_v, down_v, arrived, hidden, near_back, far_sum, tokens, picked, relay_back,
    meta_v, chosen_t, relay_weights, stream_v, total,
    gate_sem, up_sem, down_sem, tok_send, tok_recv, meta_send, meta_recv,
    near_send, near_recv, pick_send, pick_recv, back_send, back_recv,
    far_send, far_recv, sum_send, sum_recv, own_sem,
):
    me = lax.axis_index("sp")
    quarter, half = n // 4, n // 2
    plane, spot = me // quarter, me % quarter
    side = plane // 2
    relaying = (plane + side) % 2
    units = gate_v.shape[1]
    width = normed_hbm.shape[1]
    depth = down_v.shape[0]
    chunks = width // chunk
    down_tiles = width // down_tile
    far_relay = (2 - side) * quarter + spot
    my_turn = relaying

    def source_of(s):
        return (3 - s - (3 - 2 * s) * side) * quarter + spot

    def columns(t, size):
        return pl.ds(pl.multiple_of(t * size, size), size)

    def load(src, dst, sem, t, size):
        cols = columns(t, size)
        return pltpu.make_async_copy(src.at[0, :, cols], dst.at[:, cols], sem.at[t])

    def load_down(step):
        return pltpu.make_async_copy(
            down_hbm.at[0, :, columns(step % down_tiles, down_tile)],
            down_v.at[step % depth],
            down_sem.at[step % depth],
        )

    def remote(src, dst, sent, got, device):
        return pltpu.make_async_remote_copy(
            src_ref=src, dst_ref=dst, send_sem=sent, recv_sem=got,
            device_id={"sp": device}, device_id_type=MESH,
        )

    def settle(ref, sem):
        pltpu.make_async_copy(ref, ref, sem).wait()

    def block(i, count=1):
        return pl.ds(i * cap, count * cap)

    passes = pass_plan(n)
    pass_starts, places, first_far = [0], {}, {}
    for members, group in passes:
        for d in members:
            places[d] = pass_starts[-1] + d - members[0]
        end = pass_starts[-1] + len(members)
        if group is not None:
            first_far[group] = end
            end += quarter
        pass_starts.append(end)

    barrier = pltpu.get_barrier_semaphore()

    def on_edge(task):
        pl.when(relaying == 0)(task)

    def greet(device):
        pl.semaphore_signal(barrier, inc=1, device_id={"sp": device}, device_id_type=MESH)

    for d in range(1, half):
        greet(flipped(me, d, n))
    greet(far_relay)

    @pl.when(relaying == 1)
    def _():
        greet(source_of(0))
        greet(source_of(1))

    own_rows = pltpu.make_async_copy(rows_hbm.at[block(0)], arrived.at[block(0)], own_sem.at[0])
    own_rows.start()
    for t in range(units // tile):
        load(gate_hbm, gate_v, gate_sem, t, tile).start()
        load(up_hbm, up_v, up_sem, t, tile).start()
    for t in range(depth):
        load_down(t).start()
    stream_in = pltpu.make_async_copy(stream_hbm, stream_v, own_sem.at[1])
    stream_in.start()
    pl.semaphore_wait(barrier, half + 2 * relaying)

    def send_tokens():
        remote(
            meta_hbm, meta_v.at[my_turn], meta_send.at[0], meta_recv.at[my_turn], far_relay
        ).start()
        for c in range(chunks):
            cols = pl.ds(c * chunk, chunk)
            remote(
                normed_hbm.at[:, cols], tokens.at[my_turn, :, cols],
                tok_send.at[0], tok_recv.at[my_turn * chunks + c], far_relay,
            ).start()

    def send_near(distances):
        for d in distances:
            remote(
                rows_hbm.at[block(d)], arrived.at[block(places[d])],
                near_send.at[0], near_recv.at[d // quarter], flipped(me, d, n),
            ).start()

    middle = quarter + quarter // 2
    send_tokens()
    send_near(range(1, middle))
    on_edge(lambda: send_near(range(middle, half)))

    def pick(s, c):
        cols = columns(c, chunk)
        settle(tokens.at[s, :, cols], tok_recv.at[s * chunks + c])
        if s > 0:
            settle(picked.at[block(1, half - 1), cols], pick_send.at[c])
        rows = jnp.dot(
            chosen_t[...], tokens[s, :, cols], preferred_element_type=jnp.float32
        ).astype(jnp.bfloat16)
        arrived[block(first_far[s]), cols] = rows[:cap]
        picked[pl.ds(cap, (half - 1) * cap), cols] = rows[cap:]
        for d in list(range(quarter, half)) + list(range(1, quarter)):
            remote(
                picked.at[block(d), cols],
                arrived.at[block(first_far[s] + d % quarter), cols],
                pick_send.at[c], pick_recv.at[s * chunks + c], flipped(me, d, n),
            ).start()

    def read_meta(s):
        settle(meta_v.at[s], meta_recv.at[s])
        places = meta_v[s, :half].astype(jnp.bfloat16)
        shares = meta_v[s, half:].astype(jnp.bfloat16)
        chosen_t[...] = (
            jnp.dot(spread_t[...], places, preferred_element_type=jnp.float32) == wanted_col[...]
        ).astype(jnp.float32).astype(jnp.bfloat16)
        across = (((0,), (0,)), ((), ()))
        slots = lax.dot_general(places, spread_v[...], across, preferred_element_type=jnp.float32)
        spread_shares = lax.dot_general(
            shares, spread_v[...], across, preferred_element_type=jnp.float32
        )
        relay_weights[s] = jnp.where(slots == wanted_row[...], spread_shares, 0.0).astype(
            jnp.bfloat16
        )

    def relay_sum(s, c):
        cols = columns(c, chunk)
        settle(relay_back.at[s, block(1, half - 1), cols], far_recv.at[s * chunks + c])
        tokens[s, :, cols] = jnp.dot(
            relay_weights[s], relay_back[s, :, cols], preferred_element_type=jnp.float32
        ).astype(jnp.bfloat16)
        remote(
            tokens.at[s, :, cols], far_sum.at[:, cols], sum_send.at[0], sum_recv.at[c], source_of(s)
        ).start()

    def on_relay(task):
        pl.when(relaying == 1)(task)

    def experts(g, amid=(), between=None, amid_down=()):
        first, after = pass_starts[g], pass_starts[g + 1]
        rows = block(first, after - first)
        used = pl.ds(0, (after - first) * cap)
        s = passes[g][1]
        far = s is not None
        own_far = len(passes[g][0]) * cap
        has_own = 0 in passes[g][0]

        @pl.loop(0, units // tile)
        def _(t):
            for when, role, task in amid:
                here = (t == when) if role is None else (relaying == role) & (t == when)
                pl.when(here)(task)
            if g == 0:
                load(gate_hbm, gate_v, gate_sem, t, tile).wait()
                load(up_hbm, up_v, up_sem, t, tile).wait()
            cols = columns(t, tile)
            x = arrived[rows, :]
            gate = jnp.dot(x, gate_v[:, cols], preferred_element_type=jnp.float32)
            up = jnp.dot(x, up_v[:, cols], preferred_element_type=jnp.float32)
            hidden[used, cols] = (gate / (1.0 + jnp.exp(-gate)) * up).astype(jnp.bfloat16)

        if between is not None:
            between()

        @pl.loop(0, down_tiles)
        def _(t):
            step = g * down_tiles + t
            for when, role, task in amid_down:
                here = (t == when) if role is None else (relaying == role) & (t == when)
                pl.when(here)(task)
            load_down(step).wait()
            cols = columns(t, down_tile)
            result = jnp.dot(
                hidden[used, :], down_v[step % depth], preferred_element_type=jnp.float32
            ).astype(jnp.bfloat16)
            arrived[rows, cols] = result
            if has_own:
                near_back[block(0), cols] = result[:cap]

            if far:
                @pl.when(relaying == 1)
                def _():
                    relay_back[s, block(0), cols] = result[own_far:own_far + cap]

            @pl.when(step + depth < len(passes) * down_tiles)
            def _():
                load_down(step + depth).start()

            if far:
                per = chunk // down_tile

                @pl.when(t % per == per - 1)
                def _():
                    c = t // per
                    if s == 0:
                        on_edge(lambda: give_far(s, c, range(quarter)))
                    else:
                        on_edge(lambda: give_far(s, c, range(1)))
                        give_far(s, c, range(1, quarter))

    def give_far(s, c, spots):
        wide = columns(c, chunk)
        for p in spots:
            target = (1 + side) * quarter + flipped(spot, p, quarter)
            place = pl.multiple_of((p + quarter * (1 - relaying)) * cap, cap)
            remote(
                arrived.at[block(first_far[s] + p), wide],
                relay_back.at[s, pl.ds(place, cap), wide],
                far_send.at[s], far_recv.at[s * chunks + c], target,
            ).start()

    def near_distances(i):
        return range(max(1, i * quarter), (i + 1) * quarter)

    def near_part(ref, i, places):
        members = near_distances(i)
        return ref.at[block(places[members[0]], len(members))]

    def give_near(distances):
        for d in distances:
            i = d // quarter
            remote(
                arrived.at[block(places[d])], near_back.at[block(d)],
                back_send.at[i], back_recv.at[i], flipped(me, d, n),
            ).start()

    plain = {d: d for d in range(half)}

    def first_pick():
        read_meta(0)
        pick(0, 0)

    on_relay(first_pick)
    own_rows.wait()
    settle(near_part(arrived, 0, places), near_recv.at[0])
    experts(
        0, amid=[(8, 1, lambda: pick(0, 1))],
        amid_down=[(0, 1, lambda: pick(0, 2))],
    )

    def last_of_first():
        pick(0, chunks - 1)
        send_near(range(middle, half))

    on_relay(last_of_first)

    def await_far(s):
        first = first_far[s]

        @pl.when(relaying == 1)
        def _():
            for c in range(chunks):
                cols = pl.ds(c * chunk, chunk)
                settle(arrived.at[block(first + 1, quarter - 1), cols], pick_recv.at[s * chunks + c])

        @pl.when(relaying == 0)
        def _():
            for c in range(chunks):
                cols = pl.ds(c * chunk, chunk)
                settle(arrived.at[block(first, quarter), cols], pick_recv.at[s * chunks + c])

    def first_of_second():
        read_meta(1)
        pick(1, 0)

    await_far(0)
    experts(
        1, amid=[(5, 1, first_of_second), (14, 1, lambda: pick(1, 1))],
        amid_down=[(6, 1, lambda: pick(1, 2))],
    )
    def last_of_second():
        pick(1, chunks - 1)
        for c in range(chunks):
            give_far(0, c, range(1, quarter))

    settle(near_part(arrived, 1, places), near_recv.at[1])
    experts(
        2, amid=[
            (1, 1, last_of_second), (12, 1, lambda: relay_sum(0, 0)),
            (15, 1, lambda: relay_sum(0, 1)),
        ],
        amid_down=[(4, 1, lambda: relay_sum(0, 2))],
    )
    on_relay(lambda: relay_sum(0, 3))

    def relay_sums(s):
        @pl.loop(0, chunks)
        def _(c):
            relay_sum(s, c)

    await_far(1)
    experts(3, amid=[(7, None, lambda: give_near(range(middle, half)))])
    give_near(range(1, middle))
    on_relay(lambda: relay_sums(1))
    for i in range(2):
        settle(near_part(near_back, i, plain), back_recv.at[i])

    @pl.loop(0, chunks)
    def _(c):
        cols = columns(c, chunk)
        total[:, cols] = jnp.dot(
            weights_v[...], near_back[:, cols], preferred_element_type=jnp.float32
        )

    stream_in.wait()
    for c in range(chunks):
        cols = pl.ds(c * chunk, chunk)
        settle(far_sum.at[:, cols], sum_recv.at[c])

    part = 32

    @pl.loop(0, total.shape[0] // part)
    def _(t):
        some = pl.ds(pl.multiple_of(t * part, part), part)
        combined = total[some, :] + far_sum[some, :].astype(jnp.float32)
        out_v[some, :] = (stream_v[some, :] + rms_scale(combined, gain_v[...])).astype(out_v.dtype)

    settle(normed_hbm, tok_send.at[0])
    settle(meta_hbm, meta_send.at[0])
    settle(rows_hbm.at[block(1, half - 1)], near_send.at[0])
    for i in range(2):
        settle(near_part(arrived, i, places), back_send.at[i])

    @pl.when(relaying == 1)
    def _():
        for c in range(chunks):
            settle(picked.at[block(1, half - 1), pl.ds(c * chunk, chunk)], pick_send.at[c])
        settle(tokens, sum_send.at[0])
        for s in range(2):
            settle(arrived.at[block(first_far[s] + 1, quarter - 1)], far_send.at[s])

    @pl.when(relaying == 0)
    def _():
        for s in range(2):
            settle(arrived.at[block(first_far[s], quarter)], far_send.at[s])


def run_experts(outgoing, normed, meta, w_gate, w_up, w_down, weights, stream, gain, n, cap):
    model_width, units = w_gate.shape[1], w_gate.shape[2]
    rows_blk = normed.shape[0]
    tile, down_tile, chunk, depth = 256, 256, model_width // 4, 4
    half, chunks = n // 2, 4
    total_rows = n * cap
    longest = max(len(m) + (0 if s is None else n // 4) for m, s in pass_plan(n))
    slots = np.arange(half * cap)
    spread = (slots[None, :] // cap == np.arange(half)[:, None]).astype(np.float32)
    wanted = (slots % cap + 1).astype(np.float32)
    constants = (
        jnp.asarray(spread, jnp.bfloat16),
        jnp.asarray(spread.T, jnp.bfloat16),
        jnp.asarray(wanted[None, :]),
        jnp.asarray(wanted[:, None]),
    )
    dma = pltpu.SemaphoreType.DMA
    vmem = pltpu.VMEM
    anywhere = pl.BlockSpec(memory_space=pl.ANY)
    near = pl.BlockSpec(memory_space=pltpu.VMEM)
    return pl.pallas_call(
        functools.partial(expert_kernel, n, cap, tile, down_tile, chunk),
        out_shape=jax.ShapeDtypeStruct(stream.shape, jnp.bfloat16),
        in_specs=[anywhere] * 6 + [near] * 5 + [anywhere, near],
        out_specs=near,
        scratch_shapes=[
            vmem((model_width, units), jnp.bfloat16),
            vmem((model_width, units), jnp.bfloat16),
            vmem((depth, units, down_tile), jnp.bfloat16),
            vmem((total_rows, model_width), jnp.bfloat16),
            vmem((longest * cap, units), jnp.bfloat16),
            vmem((half * cap, model_width), jnp.bfloat16),
            vmem((rows_blk, model_width), jnp.bfloat16),
            vmem((2, rows_blk, model_width), jnp.bfloat16),
            vmem((half * cap, model_width), jnp.bfloat16),
            vmem((2, half * cap, model_width), jnp.bfloat16),
            vmem((2,) + meta.shape, jnp.float32),
            vmem((half * cap, rows_blk), jnp.bfloat16),
            vmem((2, rows_blk, half * cap), jnp.bfloat16),
            vmem(stream.shape, jnp.float32),
            vmem(stream.shape, jnp.float32),
            dma((units // tile,)),
            dma((units // tile,)),
            dma((depth,)),
            dma((1,)),
            dma((2 * chunks,)),
            dma((1,)),
            dma((2,)),
            dma((1,)),
            dma((3,)),
            dma((chunks,)),
            dma((2 * chunks,)),
            dma((3,)),
            dma((3,)),
            dma((2,)),
            dma((2 * chunks,)),
            dma((1,)),
            dma((chunks,)),
            dma((2,)),
        ],
        compiler_params=pltpu.CompilerParams(
            collective_id=0, has_side_effects=True, vmem_limit_bytes=67043328
        ),
        cost_estimate=pl.CostEstimate(
            flops=6 * total_rows * model_width * units,
            bytes_accessed=6 * model_width * units,
            transcendentals=total_rows * units,
        ),
    )(outgoing, normed, meta, w_gate, w_up, w_down, weights, *constants, stream, gain)


def per_device_whole(
    resid, gate_b, gate_c, value, taps, doc_ids, out_weight, norm_gains,
    routes, route_weights, w_gate, w_up, w_down,
):
    tok_dev = gate_b.shape[0]
    rows_blk, model_width = resid.shape
    experts = lax.axis_size("sp")
    capacity = max(2, 3 * TOP * rows_blk // (2 * experts))
    tap_reach = TAPS - 1
    product = gate_c.astype(jnp.float32) * value.astype(jnp.float32)
    id_values = doc_ids.astype(jnp.float32)
    id_row = jnp.pad(id_values[tok_dev - tap_reach :], (0, model_width - tap_reach))
    handed = passed_along(
        jnp.concatenate([product[tok_dev - tap_reach :], id_row[None]], axis=0), "sp", 1
    )
    ext_rows = jnp.concatenate([handed[:tap_reach], product], axis=0)
    ext_ids = jnp.concatenate([handed[tap_reach, :tap_reach], id_values], axis=0)
    tap_weights = taps.astype(jnp.float32)
    convolved = tap_weights[0] * product
    for distance in range(1, TAPS):
        earlier = ext_rows[tap_reach - distance : tap_reach - distance + tok_dev]
        same_doc = ext_ids[tap_reach - distance : tap_reach - distance + tok_dev] == id_values
        convolved = convolved + jnp.where(same_doc[:, None], tap_weights[distance] * earlier, 0.0)
    mixed_rows = (gate_b.astype(jnp.float32) * convolved).astype(jnp.bfloat16)
    projected = (
        jnp.dot(mixed_rows, out_weight, preferred_element_type=jnp.float32)
        .astype(jnp.bfloat16)
        .astype(jnp.float32)
    )
    stream = resid.astype(jnp.float32) + rms_scale(projected, norm_gains[0])
    normed = rms_scale(stream, norm_gains[1]).astype(jnp.bfloat16)

    def dot32(a, b):
        return jnp.dot(a, b, preferred_element_type=jnp.float32)

    me = lax.axis_index("sp")
    quarter, half = experts // 4, experts // 2
    plane = me // quarter
    far_relay = (2 - plane // 2) * quarter + me % quarter
    places = jnp.arange(half, dtype=jnp.int32)
    visited = jnp.concatenate([places ^ me, places ^ far_relay])
    names = routes[:, :, None] == visited[None, None, :]
    hit = jnp.any(names, axis=1)
    earlier_rows = jnp.asarray(np.tril(np.ones((rows_blk, rows_blk), np.float32), -1), jnp.bfloat16)
    rank = dot32(earlier_rows, hit.astype(jnp.bfloat16))
    place = jnp.where(hit, rank + 1.0, 0.0)
    slots = np.arange(half * capacity)
    spread = jnp.asarray(
        (slots[None, :] // capacity == np.arange(half)[:, None]).astype(np.float32), jnp.bfloat16
    )
    wanted = jnp.asarray((slots % capacity + 1).astype(np.float32))
    chosen = dot32(place[:, :half].astype(jnp.bfloat16), spread) == wanted[None, :]
    outgoing = lax.dot_general(
        chosen.astype(jnp.bfloat16),
        normed,
        (((0,), (0,)), ((), ())),
        preferred_element_type=jnp.float32,
    ).astype(jnp.bfloat16)
    shares = route_weights / jnp.sum(route_weights, axis=1, keepdims=True)
    share_of = jnp.sum(jnp.where(names, shares[:, :, None], 0.0), axis=1)
    weights = jnp.where(
        chosen, dot32(share_of[:, :half].astype(jnp.bfloat16), spread), 0.0
    ).astype(jnp.bfloat16)
    meta = jnp.concatenate([place[:, half:].T, share_of[:, half:].T], axis=0)
    return run_experts(
        outgoing, normed, meta, w_gate, w_up, w_down, weights, stream, norm_gains[2:3], experts, capacity
    )


def solution(mesh):
    experts = mesh.shape["sp"]
    whole_tokens = mesh.shape["tp"] == 1 and experts >= 8 and experts & (experts - 1) == 0
    per_device = per_device_whole if whole_tokens else per_device_split
    return jax.shard_map(
        per_device,
        mesh=mesh,
        in_specs=(
            P(("grp", "sp", "tp"), None),
            P(("grp", "sp"), "tp"),
            P(("grp", "sp"), "tp"),
            P(("grp", "sp"), "tp"),
            P(None, "tp"),
            P(("grp", "sp")),
            P("tp", None),
            P(),
            P(("grp", "sp"), None),
            P(("grp", "sp"), None),
            P("sp", None, "tp"),
            P("sp", None, "tp"),
            P("sp", "tp", None),
        ),
        out_specs=P(("grp", "sp", "tp"), None),
        check_vma=False,
    )
```

```python
import functools

import jax
import jax.numpy as jnp
import numpy as np
from jax import lax
from jax.experimental import pallas as pl
from jax.experimental.pallas import tpu as pltpu
from jax.sharding import PartitionSpec as P

TAPS = 3
TOP = 2


norm_eps = 1e-06


def passed_along(block, axis, distance):
    devices = range(lax.axis_size(axis))
    route = [(i - distance, i) for i in devices if i - distance in devices]
    return lax.ppermute(block, axis, route)


def rms_scale(values, gain_row):
    mean_sq = jnp.mean(values * values, axis=-1, keepdims=True)
    return values * lax.rsqrt(mean_sq + norm_eps) * gain_row


def slot_table(block_routes, experts, capacity):
    block_count = block_routes.shape[0]
    block_len = block_routes.shape[1]
    flat_routes = block_routes.reshape(block_count, block_len * TOP)
    onehot = (
        flat_routes[:, :, None] == jnp.arange(experts, dtype=jnp.int32)[None, None, :]
    ).astype(jnp.int32)
    before = jnp.cumsum(onehot, axis=1) - onehot
    slot_rank = jnp.sum(before * onehot, axis=2)
    slot_hit = onehot[:, :, :, None] * (
        slot_rank[:, :, None, None] == jnp.arange(capacity, dtype=jnp.int32)[None, None, None, :]
    ).astype(jnp.int32)
    owner_row = jnp.arange(block_len * TOP, dtype=jnp.int32) // TOP
    slot_tok = jnp.sum(slot_hit * owner_row[None, :, None, None], axis=1)
    filled = jnp.sum(slot_hit, axis=1)
    return (slot_rank.reshape(block_count, block_len, TOP), slot_tok, filled)


def pick_rows(normed_rows, slot_tok, filled):
    picked_rows = normed_rows[slot_tok]
    return jnp.where(filled[:, :, None] > 0, picked_rows, jnp.zeros_like(picked_rows))


def expert_hidden(picked_rows, w_gate, w_up):
    gate_proj = jnp.dot(picked_rows, w_gate[0], preferred_element_type=jnp.float32)
    up_proj = jnp.dot(picked_rows, w_up[0], preferred_element_type=jnp.float32)
    return (jax.nn.silu(gate_proj) * up_proj).astype(jnp.bfloat16)


def per_device_split(
    resid,
    gate_b,
    gate_c,
    value,
    taps,
    doc_ids,
    out_weight,
    norm_gains,
    routes,
    route_weights,
    w_gate,
    w_up,
    w_down,
):
    tok_dev = gate_b.shape[0]
    rows_blk = resid.shape[0]
    model_width = resid.shape[1]
    experts = lax.axis_size("sp")
    capacity = max(2, 3 * TOP * rows_blk // (2 * experts))
    tap_reach = TAPS - 1
    product = gate_c.astype(jnp.float32) * value.astype(jnp.float32)
    id_values = doc_ids.astype(jnp.float32)
    prev_rows, prev_ids = passed_along(
        (product[tok_dev - tap_reach :], id_values[tok_dev - tap_reach :]), "sp", 1
    )
    ext_rows = jnp.concatenate([prev_rows, product], axis=0)
    ext_ids = jnp.concatenate([prev_ids, id_values], axis=0)
    tap_weights = taps.astype(jnp.float32)
    convolved = tap_weights[0] * product
    for distance in range(1, TAPS):
        earlier = ext_rows[tap_reach - distance : tap_reach - distance + tok_dev]
        same_doc = ext_ids[tap_reach - distance : tap_reach - distance + tok_dev] == id_values
        convolved = convolved + jnp.where(same_doc[:, None], tap_weights[distance] * earlier, 0.0)
    mixed_rows = (gate_b.astype(jnp.float32) * convolved).astype(jnp.bfloat16)
    block_rows = mixed_rows
    projected = lax.psum_scatter(
        jnp.dot(block_rows, out_weight, preferred_element_type=jnp.float32).astype(jnp.bfloat16),
        "tp",
        scatter_dimension=0,
        tiled=True,
    ).astype(jnp.float32)
    stream = resid.astype(jnp.float32) + rms_scale(projected, norm_gains[0])
    normed = rms_scale(stream, norm_gains[1]).astype(jnp.bfloat16)
    lane_index = lax.axis_index("tp")
    offset = lane_index * rows_blk
    my_routes = lax.dynamic_slice_in_dim(routes, offset, rows_blk, 0)
    my_weights = lax.dynamic_slice_in_dim(route_weights, offset, rows_blk, 0)
    own_rank, own_tok, own_filled = slot_table(my_routes[None], experts, capacity)
    slot_rank = own_rank[0]
    outgoing = pick_rows(normed, own_tok[0], own_filled[0])
    arrived = lax.all_to_all(outgoing, "sp", split_axis=0, concat_axis=0, tiled=True)
    hidden = expert_hidden(
        lax.all_gather(arrived[None], "tp", axis=0, tiled=True).reshape(-1, model_width),
        w_gate,
        w_up,
    )
    block_rows = hidden
    summed = lax.psum_scatter(
        jnp.dot(block_rows, w_down[0], preferred_element_type=jnp.float32).astype(jnp.bfloat16),
        "tp",
        scatter_dimension=0,
        tiled=True,
    )
    results = summed.reshape(experts, capacity, model_width)
    returned = lax.all_to_all(results, "sp", split_axis=0, concat_axis=0, tiled=True)
    picked = returned[my_routes, slot_rank]
    shares = my_weights / jnp.sum(my_weights, axis=1, keepdims=True)
    combined = jnp.sum(shares[:, :, None] * picked.astype(jnp.float32), axis=1)
    return (stream + rms_scale(combined, norm_gains[2])).astype(jnp.bfloat16)


MESH = pl.DeviceIdType.MESH


def flipped(me, distance, n):
    out, bit = 0, 1
    while bit < n:
        digit = (me // bit) % 2
        if distance & bit:
            digit = 1 - digit
        out = out + digit * bit
        bit *= 2
    return out


def pass_plan(n):
    quarter, half = n // 4, n // 2
    return [(range(quarter), None), ((), 0), (range(quarter, half), None), ((), 1)]


def expert_kernel(
    n, cap, tile, down_tile, chunk,
    normed_hbm, meta_hbm, gate_hbm, up_hbm, down_hbm,
    near_meta, spread_v, spread_t, wanted_row, wanted_col, stream_hbm, gain_v, out_v,
    gate_v, up_v, down_v, arrived, hidden, near_rows, near_back, far_sum, tokens, picked, relay_back,
    meta_v, chosen_t, near_weights, relay_weights, stream_v, total,
    gate_sem, up_sem, down_sem, tok_send, tok_recv, meta_send, meta_recv,
    near_send, near_recv, pick_send, pick_recv, back_send, back_recv,
    far_send, far_recv, sum_send, sum_recv, own_sem,
):
    me = lax.axis_index("sp")
    quarter, half = n // 4, n // 2
    plane, spot = me // quarter, me % quarter
    side = plane // 2
    relaying = (plane + side) % 2
    units = gate_v.shape[1]
    width = normed_hbm.shape[1]
    depth = down_v.shape[0]
    chunks = width // chunk
    down_tiles = width // down_tile
    far_relay = (2 - side) * quarter + spot
    my_turn = relaying

    def source_of(s):
        return (3 - s - (3 - 2 * s) * side) * quarter + spot

    def columns(t, size):
        return pl.ds(pl.multiple_of(t * size, size), size)

    def load(src, dst, sem, t, size):
        cols = columns(t, size)
        return pltpu.make_async_copy(src.at[0, :, cols], dst.at[:, cols], sem.at[t])

    def load_down(step):
        return pltpu.make_async_copy(
            down_hbm.at[0, :, columns(step % down_tiles, down_tile)],
            down_v.at[step % depth],
            down_sem.at[step % depth],
        )

    def remote(src, dst, sent, got, device):
        return pltpu.make_async_remote_copy(
            src_ref=src, dst_ref=dst, send_sem=sent, recv_sem=got,
            device_id={"sp": device}, device_id_type=MESH,
        )

    def settle(ref, sem):
        pltpu.make_async_copy(ref, ref, sem).wait()

    def block(i, count=1):
        return pl.ds(i * cap, count * cap)

    passes = pass_plan(n)
    pass_starts, places, first_far = [0], {}, {}
    for members, group in passes:
        for d in members:
            places[d] = pass_starts[-1] + d - members[0]
        end = pass_starts[-1] + len(members)
        if group is not None:
            first_far[group] = end
            end += quarter
        pass_starts.append(end)

    barrier = pltpu.get_barrier_semaphore()

    def on_edge(task):
        pl.when(relaying == 0)(task)

    def greet(device):
        pl.semaphore_signal(barrier, inc=1, device_id={"sp": device}, device_id_type=MESH)

    for d in range(1, half):
        greet(flipped(me, d, n))
    greet(far_relay)

    @pl.when(relaying == 1)
    def _():
        greet(source_of(0))
        greet(source_of(1))

    normed_in = pltpu.make_async_copy(normed_hbm, far_sum, own_sem.at[0])
    normed_in.start()

    def select(meta, weights_ref):
        places = meta[:half].astype(jnp.bfloat16)
        shares = meta[half:].astype(jnp.bfloat16)
        chosen_t[...] = (
            jnp.dot(spread_t[...], places, preferred_element_type=jnp.float32) == wanted_col[...]
        ).astype(jnp.float32).astype(jnp.bfloat16)
        across = (((0,), (0,)), ((), ()))
        slots = lax.dot_general(places, spread_v[...], across, preferred_element_type=jnp.float32)
        spread_shares = lax.dot_general(
            shares, spread_v[...], across, preferred_element_type=jnp.float32
        )
        weights_ref[...] = jnp.where(slots == wanted_row[...], spread_shares, 0.0).astype(
            jnp.bfloat16
        )

    select(near_meta[...], near_weights)
    normed_in.wait()
    for t in range(units // tile):
        load(gate_hbm, gate_v, gate_sem, t, tile).start()
        load(up_hbm, up_v, up_sem, t, tile).start()
    for t in range(depth):
        load_down(t).start()
    stream_in = pltpu.make_async_copy(stream_hbm, stream_v, own_sem.at[1])
    stream_in.start()

    @pl.loop(0, chunks)
    def _(c):
        cols = columns(c, chunk)
        rows = jnp.dot(
            chosen_t[...], far_sum[:, cols], preferred_element_type=jnp.float32
        ).astype(jnp.bfloat16)
        arrived[block(0), cols] = rows[:cap]
        near_rows[:, cols] = rows[cap:]

    pl.semaphore_wait(barrier, half + 2 * relaying)

    def send_tokens():
        remote(
            meta_hbm, meta_v.at[my_turn], meta_send.at[0], meta_recv.at[my_turn], far_relay
        ).start()
        for c in range(chunks):
            cols = pl.ds(c * chunk, chunk)
            remote(
                normed_hbm.at[:, cols], tokens.at[my_turn, :, cols],
                tok_send.at[0], tok_recv.at[my_turn * chunks + c], far_relay,
            ).start()

    def send_near(distances):
        for d in distances:
            remote(
                near_rows.at[block(d - 1)], arrived.at[block(places[d])],
                near_send.at[0], near_recv.at[d // quarter], flipped(me, d, n),
            ).start()

    middle = quarter + quarter // 2
    send_tokens()
    send_near(range(1, middle))
    on_edge(lambda: send_near(range(middle, half)))

    def pick(s, c):
        cols = columns(c, chunk)
        settle(tokens.at[s, :, cols], tok_recv.at[s * chunks + c])
        if s > 0:
            settle(picked.at[block(1, half - 1), cols], pick_send.at[c])
        rows = jnp.dot(
            chosen_t[...], tokens[s, :, cols], preferred_element_type=jnp.float32
        ).astype(jnp.bfloat16)
        arrived[block(first_far[s]), cols] = rows[:cap]
        picked[pl.ds(cap, (half - 1) * cap), cols] = rows[cap:]
        for d in list(range(quarter, half)) + list(range(1, quarter)):
            remote(
                picked.at[block(d), cols],
                arrived.at[block(first_far[s] + d % quarter), cols],
                pick_send.at[c], pick_recv.at[s * chunks + c], flipped(me, d, n),
            ).start()

    def read_meta(s):
        settle(meta_v.at[s], meta_recv.at[s])
        select(meta_v[s], relay_weights.at[s])

    def relay_sum(s, c):
        cols = columns(c, chunk)
        settle(relay_back.at[s, block(1, half - 1), cols], far_recv.at[s * chunks + c])
        tokens[s, :, cols] = jnp.dot(
            relay_weights[s], relay_back[s, :, cols], preferred_element_type=jnp.float32
        ).astype(jnp.bfloat16)
        remote(
            tokens.at[s, :, cols], far_sum.at[:, cols], sum_send.at[0], sum_recv.at[c], source_of(s)
        ).start()

    def on_relay(task):
        pl.when(relaying == 1)(task)

    def extent(g):
        first, after = pass_starts[g], pass_starts[g + 1]
        return block(first, after - first), pl.ds(0, (after - first) * cap)

    def gate_up(g, slot, amid=()):
        rows, used = extent(g)

        @pl.loop(0, units // tile)
        def _(t):
            for when, role, task in amid:
                here = (t == when) if role is None else (relaying == role) & (t == when)
                pl.when(here)(task)
            if g == 0:
                load(gate_hbm, gate_v, gate_sem, t, tile).wait()
                load(up_hbm, up_v, up_sem, t, tile).wait()
            cols = columns(t, tile)
            x = arrived[rows, :]
            gate = jnp.dot(x, gate_v[:, cols], preferred_element_type=jnp.float32)
            up = jnp.dot(x, up_v[:, cols], preferred_element_type=jnp.float32)
            hidden[slot, used, cols] = (gate / (1.0 + jnp.exp(-gate)) * up).astype(jnp.bfloat16)

    def down(g, slot, turn, amid_down=()):
        rows, used = extent(g)
        s = passes[g][1]
        far = s is not None
        own_far = len(passes[g][0]) * cap
        has_own = 0 in passes[g][0]

        @pl.loop(0, down_tiles)
        def _(t):
            step = turn * down_tiles + t
            for when, role, task in amid_down:
                here = (t == when) if role is None else (relaying == role) & (t == when)
                pl.when(here)(task)
            load_down(step).wait()
            cols = columns(t, down_tile)
            result = jnp.dot(
                hidden[slot, used, :], down_v[step % depth], preferred_element_type=jnp.float32
            ).astype(jnp.bfloat16)
            arrived[rows, cols] = result
            if has_own:
                near_back[block(0), cols] = result[:cap]

            if far:
                @pl.when(relaying == 1)
                def _():
                    relay_back[s, block(0), cols] = result[own_far:own_far + cap]

            @pl.when(step + depth < len(passes) * down_tiles)
            def _():
                load_down(step + depth).start()

            if far:
                per = chunk // down_tile

                @pl.when(t % per == per - 1)
                def _():
                    c = t // per
                    if s == 0:
                        on_edge(lambda: give_far(s, c, range(quarter)))
                    else:
                        on_edge(lambda: give_far(s, c, range(1)))
                        give_far(s, c, range(1, quarter))

    def give_far(s, c, spots):
        wide = columns(c, chunk)
        for p in spots:
            target = (1 + side) * quarter + flipped(spot, p, quarter)
            place = pl.multiple_of((p + quarter * (1 - relaying)) * cap, cap)
            remote(
                arrived.at[block(first_far[s] + p), wide],
                relay_back.at[s, pl.ds(place, cap), wide],
                far_send.at[s], far_recv.at[s * chunks + c], target,
            ).start()

    def near_distances(i):
        return range(max(1, i * quarter), (i + 1) * quarter)

    def near_part(ref, i, places):
        members = near_distances(i)
        return ref.at[block(places[members[0]], len(members))]

    def give_near(distances):
        for d in distances:
            i = d // quarter
            remote(
                arrived.at[block(places[d])], near_back.at[block(d)],
                back_send.at[i], back_recv.at[i], flipped(me, d, n),
            ).start()

    plain = {d: d for d in range(half)}

    def first_pick():
        read_meta(0)
        pick(0, 0)

    on_relay(first_pick)
    settle(near_part(arrived, 0, places), near_recv.at[0])
    gate_up(0, 0, [(8, 1, lambda: pick(0, 1))])
    down(0, 0, 0, [(0, 1, lambda: pick(0, 2))])

    def last_of_first():
        pick(0, chunks - 1)
        send_near(range(middle, half))

    on_relay(last_of_first)

    def await_far(s):
        first = first_far[s]

        @pl.when(relaying == 1)
        def _():
            for c in range(chunks):
                cols = pl.ds(c * chunk, chunk)
                settle(arrived.at[block(first + 1, quarter - 1), cols], pick_recv.at[s * chunks + c])

        @pl.when(relaying == 0)
        def _():
            for c in range(chunks):
                cols = pl.ds(c * chunk, chunk)
                settle(arrived.at[block(first, quarter), cols], pick_recv.at[s * chunks + c])

    def first_of_second():
        read_meta(1)
        pick(1, 0)

    await_far(0)
    gate_up(1, 0, [(5, 1, first_of_second), (14, 1, lambda: pick(1, 1))])
    down(1, 0, 1, [(6, 1, lambda: pick(1, 2))])

    def last_of_second():
        for c in range(2):
            give_far(0, c, range(1, quarter))
        pick(1, chunks - 1)
        for c in range(2, chunks):
            give_far(0, c, range(1, quarter))

    settle(near_part(arrived, 1, places), near_recv.at[1])
    gate_up(2, 0, [(1, 1, last_of_second)])
    down(2, 0, 2, [(2, 1, lambda: relay_sum(0, 0))])

    def relay_sums(s, first):
        @pl.loop(first, chunks)
        def _(c):
            relay_sum(s, c)

    await_far(1)
    gate_up(
        3, 0,
        [(6 * c - 5, 1, functools.partial(relay_sum, 0, c)) for c in range(1, chunks)]
        + [(9, None, lambda: give_near(range(middle, half)))],
    )
    down(3, 0, 3)
    give_near(list(range(quarter, middle)) + list(range(1, quarter)))
    on_relay(lambda: relay_sums(1, 0))
    for i in range(2):
        settle(near_part(near_back, i, plain), back_recv.at[i])

    @pl.loop(0, chunks)
    def _(c):
        cols = columns(c, chunk)
        total[:, cols] = jnp.dot(
            near_weights[...], near_back[:, cols], preferred_element_type=jnp.float32
        )

    stream_in.wait()
    for c in range(chunks):
        cols = pl.ds(c * chunk, chunk)
        settle(far_sum.at[:, cols], sum_recv.at[c])

    part = 32

    @pl.loop(0, out_v.shape[0] // part)
    def _(t):
        some = pl.ds(pl.multiple_of(t * part, part), part)
        combined = total[some, :] + far_sum[some, :].astype(jnp.float32)
        out_v[some, :] = (stream_v[some, :] + rms_scale(combined, gain_v[...])).astype(out_v.dtype)

    settle(normed_hbm, tok_send.at[0])
    settle(meta_hbm, meta_send.at[0])
    settle(near_rows, near_send.at[0])
    for i in range(2):
        settle(near_part(arrived, i, places), back_send.at[i])

    @pl.when(relaying == 1)
    def _():
        for c in range(chunks):
            settle(picked.at[block(1, half - 1), pl.ds(c * chunk, chunk)], pick_send.at[c])
        settle(tokens, sum_send.at[0])
        for s in range(2):
            settle(arrived.at[block(first_far[s] + 1, quarter - 1)], far_send.at[s])

    @pl.when(relaying == 0)
    def _():
        for s in range(2):
            settle(arrived.at[block(first_far[s], quarter)], far_send.at[s])


def run_experts(normed, near_meta, meta, w_gate, w_up, w_down, stream, gain, n, cap):
    model_width, units = w_gate.shape[1], w_gate.shape[2]
    rows_blk = normed.shape[0]
    tile, down_tile, chunk, depth = 256, 256, model_width // 4, 4
    half, chunks = n // 2, 4
    total_rows = n * cap
    longest = max(len(m) + (0 if s is None else n // 4) for m, s in pass_plan(n))
    slots = np.arange(half * cap)
    spread = (slots[None, :] // cap == np.arange(half)[:, None]).astype(np.float32)
    wanted = (slots % cap + 1).astype(np.float32)
    constants = (
        jnp.asarray(spread, jnp.bfloat16),
        jnp.asarray(spread.T, jnp.bfloat16),
        jnp.asarray(wanted[None, :]),
        jnp.asarray(wanted[:, None]),
    )
    dma = pltpu.SemaphoreType.DMA
    vmem = pltpu.VMEM
    anywhere = pl.BlockSpec(memory_space=pl.ANY)
    near = pl.BlockSpec(memory_space=pltpu.VMEM)
    return pl.pallas_call(
        functools.partial(expert_kernel, n, cap, tile, down_tile, chunk),
        out_shape=jax.ShapeDtypeStruct(stream.shape, jnp.bfloat16),
        in_specs=[anywhere] * 5 + [near] * 5 + [anywhere, near],
        out_specs=near,
        scratch_shapes=[
            vmem((model_width, units), jnp.bfloat16),
            vmem((model_width, units), jnp.bfloat16),
            vmem((depth, units, down_tile), jnp.bfloat16),
            vmem((total_rows, model_width), jnp.bfloat16),
            vmem((1, longest * cap, units), jnp.bfloat16),
            vmem(((half - 1) * cap, model_width), jnp.bfloat16),
            vmem((half * cap, model_width), jnp.bfloat16),
            vmem((rows_blk, model_width), jnp.bfloat16),
            vmem((2, rows_blk, model_width), jnp.bfloat16),
            vmem((half * cap, model_width), jnp.bfloat16),
            vmem((2, half * cap, model_width), jnp.bfloat16),
            vmem((2,) + meta.shape, jnp.float32),
            vmem((half * cap, rows_blk), jnp.bfloat16),
            vmem((rows_blk, half * cap), jnp.bfloat16),
            vmem((2, rows_blk, half * cap), jnp.bfloat16),
            vmem(stream.shape, jnp.float32),
            vmem(stream.shape, jnp.float32),
            dma((units // tile,)),
            dma((units // tile,)),
            dma((depth,)),
            dma((1,)),
            dma((2 * chunks,)),
            dma((1,)),
            dma((2,)),
            dma((1,)),
            dma((3,)),
            dma((chunks,)),
            dma((2 * chunks,)),
            dma((3,)),
            dma((3,)),
            dma((2,)),
            dma((2 * chunks,)),
            dma((1,)),
            dma((chunks,)),
            dma((2,)),
        ],
        compiler_params=pltpu.CompilerParams(
            collective_id=0, has_side_effects=True, vmem_limit_bytes=67043328
        ),
        cost_estimate=pl.CostEstimate(
            flops=6 * total_rows * model_width * units,
            bytes_accessed=6 * model_width * units,
            transcendentals=total_rows * units,
        ),
    )(normed, meta, w_gate, w_up, w_down, near_meta, *constants, stream, gain)


def per_device_whole(
    resid, gate_b, gate_c, value, taps, doc_ids, out_weight, norm_gains,
    routes, route_weights, w_gate, w_up, w_down,
):
    tok_dev = gate_b.shape[0]
    rows_blk, model_width = resid.shape
    experts = lax.axis_size("sp")
    capacity = max(2, 3 * TOP * rows_blk // (2 * experts))
    tap_reach = TAPS - 1
    product = gate_c.astype(jnp.float32) * value.astype(jnp.float32)
    id_values = doc_ids.astype(jnp.float32)
    id_row = jnp.pad(id_values[tok_dev - tap_reach :], (0, model_width - tap_reach))
    handed = passed_along(
        jnp.concatenate([product[tok_dev - tap_reach :], id_row[None]], axis=0), "sp", 1
    )
    ext_rows = jnp.concatenate([handed[:tap_reach], product], axis=0)
    ext_ids = jnp.concatenate([handed[tap_reach, :tap_reach], id_values], axis=0)
    tap_weights = taps.astype(jnp.float32)
    convolved = tap_weights[0] * product
    for distance in range(1, TAPS):
        earlier = ext_rows[tap_reach - distance : tap_reach - distance + tok_dev]
        same_doc = ext_ids[tap_reach - distance : tap_reach - distance + tok_dev] == id_values
        convolved = convolved + jnp.where(same_doc[:, None], tap_weights[distance] * earlier, 0.0)
    mixed_rows = (gate_b.astype(jnp.float32) * convolved).astype(jnp.bfloat16)
    projected = (
        jnp.dot(mixed_rows, out_weight, preferred_element_type=jnp.float32)
        .astype(jnp.bfloat16)
        .astype(jnp.float32)
    )
    stream = resid.astype(jnp.float32) + rms_scale(projected, norm_gains[0])
    normed = rms_scale(stream, norm_gains[1]).astype(jnp.bfloat16)

    def dot32(a, b):
        return jnp.dot(a, b, preferred_element_type=jnp.float32)

    me = lax.axis_index("sp")
    quarter, half = experts // 4, experts // 2
    plane = me // quarter
    far_relay = (2 - plane // 2) * quarter + me % quarter
    places = jnp.arange(half, dtype=jnp.int32)
    visited = jnp.concatenate([places ^ me, places ^ far_relay])
    names = routes[:, :, None] == visited[None, None, :]
    hit = jnp.any(names, axis=1)
    earlier_rows = jnp.asarray(np.tril(np.ones((rows_blk, rows_blk), np.float32), -1), jnp.bfloat16)
    rank = dot32(earlier_rows, hit.astype(jnp.bfloat16))
    place = jnp.where(hit, rank + 1.0, 0.0)
    shares = route_weights / jnp.sum(route_weights, axis=1, keepdims=True)
    share_of = jnp.sum(jnp.where(names, shares[:, :, None], 0.0), axis=1)
    meta = jnp.concatenate([place.T, share_of.T], axis=0).reshape(2, 2, half, rows_blk)
    near_meta = meta[:, 0].reshape(2 * half, rows_blk)
    far_meta = meta[:, 1].reshape(2 * half, rows_blk)
    return run_experts(
        normed, near_meta, far_meta, w_gate, w_up, w_down, stream, norm_gains[2:3], experts, capacity
    )


def solution(mesh):
    experts = mesh.shape["sp"]
    whole_tokens = mesh.shape["tp"] == 1 and experts >= 8 and experts & (experts - 1) == 0
    per_device = per_device_whole if whole_tokens else per_device_split
    return jax.shard_map(
        per_device,
        mesh=mesh,
        in_specs=(
            P(("grp", "sp", "tp"), None),
            P(("grp", "sp"), "tp"),
            P(("grp", "sp"), "tp"),
            P(("grp", "sp"), "tp"),
            P(None, "tp"),
            P(("grp", "sp")),
            P("tp", None),
            P(),
            P(("grp", "sp"), None),
            P(("grp", "sp"), None),
            P("sp", None, "tp"),
            P("sp", None, "tp"),
            P("sp", "tp", None),
        ),
        out_specs=P(("grp", "sp", "tp"), None),
        check_vma=False,
    )
```
